32 devices in a mesh: sp: 16 (over z, y, core), tp: 2 (over x).
Axes of the slice: x: 2, y: 2, z: 4, core: 2. Of those that a mesh axis runs over, the one named last changes fastest.
Arguments:
- queries: bfloat16 [8192, 1024], P('sp', 'tp'), may hold values from -40 to 40
- keys_values: bfloat16 [8192, 4, 128], P('sp', 'tp'), may hold values from -40 to 40
- doc_ids: int32 [8192], P('sp'), may hold values from 0 to 3, never falling along the last dimension, each value on 1 to 4096 neighbouring positions
- head_sink: float32 [16], P('tp'), may hold values from 3 to 7
- out_weight: bfloat16 [1024, 2048], replicated, may hold values from -0.1875 to 0.1875
- hidden_in: bfloat16 [8192, 2048], P(('sp', 'tp')), may hold values from -0.59765625 to 0.59765625
- norm_gain: float32 [2048], replicated, may hold values from 0.1 to 1.9
- expert_gate: bfloat16 [32, 2048, 1024], P(('sp', 'tp')), may hold values from -0.125 to 0.125
- expert_up: bfloat16 [32, 2048, 1024], P(('sp', 'tp')), may hold values from -0.125 to 0.125
- expert_down: bfloat16 [32, 1024, 2048], P(('sp', 'tp')), may hold values from -0.1875 to 0.1875
- routes: int32 [8192, 2], P(('sp', 'tp')), may hold values from 0 to 31, all different within a row; in each aligned block of 256 rows (0 to 255, 256 to 511, ...) at most 32 rows name the same one
- route_weight: float32 [8192, 2], P(('sp', 'tp')), may hold values from 0.1 to 1
Outputs:
- layer_out: bfloat16 [8192, 2048], P(('sp', 'tp'))
The draws below stay inside these ranges and needn't reach their ends.
Inputs may be any that keep to these rules, and one draw needn't show every extreme that they name: `routes`: in the rows of one device (aligned blocks of 256 tokens in order) no expert is named more than 32 times; some expert is named exactly 32 times in some blocks.
All inputs are finite; a program needn't handle non-finite values.
Results may differ from the reference program's by a relative error of at most 0.02.
Values may be sent and summed in bfloat16 or wider, within the bound.
A program may use at most 64 MiB of HBM per device.

```python
import math
import jax
import jax.numpy as jnp
import numpy as np
from jax import lax

D = 2048
HQ = 16
KVH = 4
HD = 64
FF = 1024
TOPK = 2
WIN = 128
TOK_DEV = 512
TOKENS = 8192
EXPERTS = 32
CAP = 32
DOCS = 4
N_TP = 2


def drawn_pair(key):
    base = jax.random.fold_in(key, 11)
    query_key, pair_key = jax.random.split(base, 2)
    queries = jnp.clip(jax.random.normal(query_key, (TOKENS, HQ * HD), jnp.float32), -6.0, 6.0)
    pairs = jnp.clip(jax.random.normal(pair_key, (TOKENS, KVH, 2 * HD), jnp.float32), -6.0, 6.0)
    return (queries, pairs)


def draw_queries(key, part):
    return drawn_pair(key)[0].astype(jnp.bfloat16)


def draw_keys_values(key, part):
    return drawn_pair(key)[1].astype(jnp.bfloat16)


def level_of(own_key, shape, shards, smallest, largest):
    factor_of = 1.0
    for dim, shards_of in shards:
        steps = jax.random.uniform(jax.random.fold_in(jax.random.fold_in(own_key, 6), dim), (shards_of,), jnp.float32, smallest / len(shards), largest / len(shards))
        factor_of = factor_of * jnp.repeat(jnp.exp(steps), shape[dim] // shards_of).reshape((-1,) + (1,) * (len(shape) - 1 - dim))
    return factor_of


def length_profile(number_of, total, most, slope):
    weights = [(1 << 20) // math.isqrt(rank ** slope) + 1 for rank in range(2, number_of + 1)]
    spare, given = total - most - (number_of - 1), [1] * (number_of - 1)
    while spare > 0:
        candidates = [i for i in range(number_of - 1) if given[i] < most]
        mass, left = sum([weights[i] for i in candidates]), spare
        for i in candidates:
            extra = min(most - given[i], max(1, left * weights[i] // mass), spare)
            given[i] = given[i] + extra
            spare = spare - extra
    return np.array([most] + given)


def ragged_sizes(stream_key, amount, total, most, skew):
    if amount == 2:
        one = jax.random.randint(stream_key, (), max(1, total - most), min(most, total - 1) + 1)
        return jnp.stack([one, total - one])
    tallies = jnp.asarray(length_profile(amount, total, most, skew), jnp.int32)
    pairs = (amount - 1) // 2
    donor, taker = tallies[1:1 + 2 * pairs:2], tallies[2:2 + 2 * pairs:2]
    room = jnp.minimum(donor - 1, most - taker)
    moved = jax.random.randint(jax.random.fold_in(stream_key, 1), (pairs,), 0, 1 << 20) % (room + 1)
    tallies = tallies.at[1:1 + 2 * pairs:2].set(donor - moved).at[2:2 + 2 * pairs:2].set(taker + moved)
    return tallies[jax.random.permutation(jax.random.fold_in(stream_key, 2), amount)]


def assign_block(key, own, number, rows, amount, top, limit, lean):
    sequence = jax.random.permutation(key, amount)
    heavy_load, common = load_shares(amount, rows * top, limit, lean, True), load_shares(amount, rows * top, limit, lean, False)
    places = jnp.arange(amount)

    def named(sizes, rotation):
        used = int((sizes > 0).sum())
        fixed = max(1, used // 4)
        passed = fixed + (places - fixed + rotation * (used - fixed)) % max(1, amount - fixed)
        return jnp.zeros((amount,), jnp.int32).at[sequence[jnp.where(places < fixed, places, passed)]].set(jnp.asarray(sizes, jnp.int32))

    sizes = jnp.where(number % 4 == 0, named(heavy_load, number // 4), named(common, number - number // 4 - 1))
    mixed = jax.random.permutation(jax.random.fold_in(own, 3), amount)
    source_of, receiver = mixed[0:amount // 2 * 2:2], mixed[1:amount // 2 * 2:2]
    slack = jnp.minimum(sizes[source_of] - 1, limit - sizes[receiver]) // 2
    slack = jnp.where((source_of == sequence[0]) | (receiver == sequence[0]) | (sizes[receiver] == 0), 0, jnp.maximum(slack, 0))
    passed = jax.random.randint(jax.random.fold_in(own, 4), (amount // 2,), 0, 1 << 20) % (slack + 1)
    sizes = sizes.at[source_of].add(-passed).at[receiver].add(passed)
    members = jnp.searchsorted(jnp.cumsum(sizes), jnp.arange(rows * top), side="right").astype(jnp.int32)
    grid = members.reshape(top, rows).T
    grid = grid[jax.random.permutation(jax.random.fold_in(own, 1), rows)]
    rotation = jax.random.randint(jax.random.fold_in(own, 2), (rows, 1), 0, top)
    return jnp.take_along_axis(grid, (jnp.arange(top)[None, :] + rotation) % top, axis=1)


def load_shares(amount, total, bound, lean, full):
    portions = [(1 << 20) // math.isqrt(standing ** lean) + 1 for standing in range(1, amount + 1)]
    largest = bound if full else min(bound, max(-(-total // amount), total * portions[0] // sum(portions)))
    least = 1 if total - largest >= amount - 1 else 0
    counts, surplus = [largest] + [least] * (amount - 1), total - largest - least * (amount - 1)
    while surplus > 0:
        candidates = [i for i in range(1, amount) if counts[i] < largest] or [i for i in range(1, amount) if counts[i] < bound]
        whole, remaining = sum([portions[i] for i in candidates]), surplus
        for i in candidates:
            extra = min(bound - counts[i], max(1, remaining * portions[i] // whole), surplus)
            counts[i] = counts[i] + extra
            surplus = surplus - extra
    return np.array(counts)


def normal_values(stream_key, shape, spread, reach, cuts=(), held_as=jnp.bfloat16):
    drawn = jax.random.normal(stream_key, shape, jnp.float32) * spread
    if len(cuts) > 0:
        drawn = level_of(stream_key, shape, cuts, -0.22, 0.18) * drawn
    return jnp.clip(drawn, min=-reach, max=reach).astype(held_as)


def setup_inputs(seed: int = 0) -> dict:
    seeds = jax.random.split(jax.random.key(seed), 13)
    queries = draw_queries(jax.random.fold_in(seeds[12], 71), 0)
    keys_values = draw_keys_values(jax.random.fold_in(seeds[12], 71), 0)
    doc_ids = jnp.searchsorted(jnp.cumsum(ragged_sizes(seeds[2], DOCS, TOKENS, 8 * TOK_DEV, 1)), jnp.arange(TOKENS), side="right").astype(jnp.int32)
    head_sink = jnp.clip(3.0 + 4.0 * jax.random.uniform(seeds[3], (HQ,), jnp.float32) ** level_of(seeds[3], (HQ,), ((0, 2),), -0.2, 0.2), 3.0, 7.0)
    out_weight = normal_values(seeds[4], (HQ * HD, D), (HQ * HD) ** -0.5, 0.1875)
    hidden_in = normal_values(seeds[5], (TOKENS, D), 0.1, 0.59765625, ((0, 32),))
    norm_gain = jnp.clip(1.0 + 0.18 * jax.random.normal(seeds[6], (D,), jnp.float32), 0.1, 1.9)
    expert_gate = normal_values(seeds[7], (EXPERTS, D, FF), D ** -0.5, 0.125, ((0, 32),))
    expert_up = normal_values(seeds[8], (EXPERTS, D, FF), D ** -0.5, 0.125, ((0, 32),))
    expert_down = normal_values(seeds[9], (EXPERTS, FF, D), FF ** -0.5, 0.1875, ((0, 32),))
    routes_keys = jax.random.split(jax.random.fold_in(seeds[10], 1), TOKENS // (TOK_DEV // N_TP))
    routes_turns = jax.random.permutation(jax.random.fold_in(seeds[10], 3), TOKENS // (TOK_DEV // N_TP))
    routes = jax.vmap(lambda own, number: assign_block(jax.random.fold_in(seeds[10], 2), own, number, TOK_DEV // N_TP, EXPERTS, TOPK, CAP, 1))(routes_keys, routes_turns).reshape((TOKENS, TOPK))
    route_weight = jnp.clip(jnp.exp(math.log(1.0) - 2.3025851 * jax.random.uniform(seeds[11], (TOKENS, TOPK), jnp.float32) ** level_of(seeds[11], (TOKENS, TOPK), ((0, 32),), -0.2, 0.2)), 0.1, 1.0)
    return {"queries": queries, "keys_values": keys_values, "doc_ids": doc_ids, "head_sink": head_sink, "out_weight": out_weight, "hidden_in": hidden_in, "norm_gain": norm_gain, "expert_gate": expert_gate, "expert_up": expert_up, "expert_down": expert_down, "routes": routes, "route_weight": route_weight}


def attend_all(queries, keys_values, doc_ids, head_sink):
    span_rows = math.gcd(512, TOKENS)
    span_count = TOKENS // span_rows
    group = HQ // KVH
    padded = jnp.pad(keys_values, ((WIN, WIN), (0, 0), (0, 0)))
    padded_docs = jnp.pad(doc_ids, (WIN, WIN), constant_values=-1)
    sink_logit = head_sink.astype(jnp.float32).reshape(KVH, group)[:, :, None, None]

    def one_span(span_index):
        first_row = (span_index * span_rows).astype(jnp.int32)
        q_span = lax.dynamic_slice_in_dim(queries, first_row, span_rows, 0).astype(jnp.float32)
        q_span = q_span.reshape(span_rows, KVH, group, HD)
        kv_span = lax.dynamic_slice_in_dim(padded, first_row, span_rows + 2 * WIN, 0).astype(jnp.float32)
        key_docs = lax.dynamic_slice_in_dim(padded_docs, first_row, span_rows + 2 * WIN, 0)
        query_docs = lax.dynamic_slice_in_dim(doc_ids, first_row, span_rows, 0)
        scores = jnp.einsum('qhgd,khd->hgqk', q_span, kv_span[..., :HD]) * HD ** (-0.5)
        query_pos = first_row + jnp.arange(span_rows, dtype=jnp.int32)
        key_pos = first_row - WIN + jnp.arange(span_rows + 2 * WIN, dtype=jnp.int32)
        allowed = (jnp.abs(key_pos[None, :] - query_pos[:, None]) <= WIN) & (key_docs[None, :] == query_docs[:, None])
        masked = jnp.where(allowed, scores, -1e+30)
        row_max = jnp.maximum(masked.max(-1, keepdims=True), sink_logit)
        exp_scores = jnp.where(allowed, jnp.exp(masked - row_max), 0.0)
        total_mass = exp_scores.sum(-1, keepdims=True) + jnp.exp(sink_logit - row_max)
        weights = (exp_scores / total_mass).astype(jnp.bfloat16).astype(jnp.float32)
        outcome = jnp.einsum('hgqk,khd->qhgd', weights, kv_span[..., HD:])
        return outcome.astype(jnp.bfloat16).reshape(span_rows, HQ * HD)
    attended = lax.map(one_span, jnp.arange(span_count, dtype=jnp.int32))
    return attended.reshape(TOKENS, HQ * HD)

def expert_apply(rows_in, gate_w, up_w, down_w):
    gate = jnp.dot(rows_in, gate_w, preferred_element_type=jnp.float32)
    upper = jnp.dot(rows_in, up_w, preferred_element_type=jnp.float32)
    expert_hidden = (jax.nn.silu(gate) * upper).astype(jnp.bfloat16)
    return jnp.dot(expert_hidden, down_w, preferred_element_type=jnp.float32).astype(jnp.bfloat16)

def reference(queries, keys_values, doc_ids, head_sink, out_weight, hidden_in, norm_gain, expert_gate, expert_up, expert_down, routes, route_weight):
    attended = attend_all(queries, keys_values, doc_ids, head_sink)
    projected = jnp.dot(attended, out_weight, preferred_element_type=jnp.float32)
    mid = (hidden_in.astype(jnp.float32) + projected).astype(jnp.bfloat16)
    mid_wide = mid.astype(jnp.float32)
    normed = (mid_wide * lax.rsqrt(lax.optimization_barrier(jnp.mean(mid_wide * mid_wide, axis=-1, keepdims=True)) + 1e-06) * norm_gain.astype(jnp.float32)).astype(jnp.bfloat16)
    local_rows = TOK_DEV // N_TP
    flat_routes = routes.reshape(EXPERTS, local_rows * TOPK)
    one_hot = (flat_routes[..., None] == jnp.arange(EXPERTS, dtype=jnp.int32)).astype(jnp.int32)
    slot_rank = (jnp.cumsum(one_hot, axis=1) * one_hot).sum(-1) - 1
    owner_block = jnp.arange(EXPERTS, dtype=jnp.int32)[:, None]
    slot_index = (flat_routes * (EXPERTS * CAP) + owner_block * CAP + slot_rank).reshape(-1).astype(jnp.int32)
    repeated = jnp.repeat(normed, TOPK, axis=0)
    buffer_rows = jnp.zeros((EXPERTS * EXPERTS * CAP, D), jnp.bfloat16).at[slot_index].set(repeated)

    def per_expert(pieces):
        return expert_apply(pieces[0], pieces[1], pieces[2], pieces[3])
    results = lax.map(per_expert, (buffer_rows.reshape(EXPERTS, EXPERTS * CAP, D), expert_gate, expert_up, expert_down))
    picked = results.reshape(-1, D)[slot_index].astype(jnp.float32).reshape(TOKENS, TOPK, D)
    mixture = lax.optimization_barrier(jnp.sum(picked * route_weight.astype(jnp.float32)[..., None], axis=1))
    return (mid_wide + mixture).astype(jnp.bfloat16)
```

```python
import functools

import jax
import jax.numpy as jnp
from jax import lax
from jax.experimental import pallas as pl
from jax.experimental.pallas import tpu as pltpu
from jax.sharding import PartitionSpec as P

HD = 64
WIN = 128
PLANES = 4
CUTS = 2
MESH = pl.DeviceIdType.MESH


def with_halo(cells, axis, width):
    count = lax.axis_size(axis)
    ends = count - 1
    return jnp.concatenate(
        [
            lax.ppermute(cells[-width:], axis, [(i, (i + 1) % count) for i in range(ends)]),
            cells,
            lax.ppermute(cells[:width], axis, [((i + 1) % count, i) for i in range(ends)]),
        ],
        axis=0,
    )


def place(stride, tps):
    sp = lax.axis_index("sp")
    tp = lax.axis_index("tp")
    return lax.div(sp, stride), lax.rem(sp, stride), tp, lax.rem(sp, stride) * tps + tp


def greet(z, r, tp, p, planes, stride, tps):
    peers = stride * tps
    barrier = pltpu.get_barrier_semaphore()
    for k in range(1, peers):
        pd = lax.rem(p + k, peers)
        pl.semaphore_signal(
            barrier,
            inc=1,
            device_id=(z * stride + lax.div(pd, tps), lax.rem(pd, tps)),
            device_id_type=MESH,
        )

    @pl.when(z > 0)
    def _():
        pl.semaphore_signal(
            barrier, inc=1, device_id=((z - 1) * stride + r, tp), device_id_type=MESH
        )

    @pl.when(z < planes - 1)
    def _():
        pl.semaphore_signal(
            barrier, inc=1, device_id=((z + 1) * stride + r, tp), device_id_type=MESH
        )

    beside = (z > 0).astype(jnp.int32) + (z < planes - 1).astype(jnp.int32)
    pl.semaphore_wait(barrier, peers - 1 + beside)


def slot_hits(tab, z, slots, rows):
    ids = lax.broadcasted_iota(jnp.int32, (slots, rows), 0) + z * slots
    ids = ids.astype(jnp.float32)
    return ids == tab[0:1, :], ids == tab[1:2, :]


def dispatch_kernel(
    planes, stride, tps, cap,
    x_ref, tab_ref, out_ref,
    toks, stage, zsend, zrecv, psend, precv, lsem,
):
    z, r, tp, p = place(stride, tps)
    peers = stride * tps
    rows, width = x_ref.shape
    cols = width // CUTS
    slots = peers * cap
    greet(z, r, tp, p, planes, stride, tps)

    def span(h):
        return pl.ds(pl.multiple_of(h * cols, cols), cols)

    def hop(zs, h, side):
        return pltpu.make_async_remote_copy(
            src_ref=toks.at[zs, :, span(h)],
            dst_ref=toks.at[zs, :, span(h)],
            send_sem=zsend.at[side, zs, h],
            recv_sem=zrecv.at[zs, h],
            device_id=((z + 1 - 2 * side) * stride + r, tp),
            device_id_type=MESH,
        )

    def own_hop(h, side):
        return pltpu.make_async_remote_copy(
            src_ref=x_ref.at[:, span(h)],
            dst_ref=toks.at[z, :, span(h)],
            send_sem=zsend.at[side, z, h],
            recv_sem=zrecv.at[z, h],
            device_id=((z + 1 - 2 * side) * stride + r, tp),
            device_id_type=MESH,
        )

    def plane_copy(zs, h, dest, at):
        return pltpu.make_async_remote_copy(
            src_ref=stage.at[zs, pl.ds(pl.multiple_of(dest * cap, cap), cap), span(h)],
            dst_ref=out_ref.at[zs, at, :, span(h)],
            send_sem=psend.at[zs, h, dest],
            recv_sem=precv.at[zs, h, at],
            device_id=(z * stride + lax.div(dest, tps), lax.rem(dest, tps)),
            device_id_type=MESH,
        )

    def local_copy(zs, h):
        return pltpu.make_async_copy(
            stage.at[zs, pl.ds(pl.multiple_of(p * cap, cap), cap), span(h)],
            out_ref.at[zs, p, :, span(h)],
            lsem.at[zs, h],
        )

    def pack(block, zs, h):
        tab = tab_ref[lax.rem(z - zs + planes, planes)]
        first, second = slot_hits(tab, z, slots, rows)
        pick = jnp.where(first | second, 1.0, 0.0).astype(jnp.bfloat16)
        stage[zs, :, span(h)] = jnp.dot(
            pick, block, preferred_element_type=jnp.float32
        ).astype(jnp.bfloat16)
        for k in range(1, peers):
            plane_copy(zs, h, lax.rem(p + k, peers), p).start()
        local_copy(zs, h).start()

    for h in range(CUTS):

        @pl.when(z < planes - 1)
        def _():
            own_hop(h, 0).start()

        @pl.when(z > 0)
        def _():
            own_hop(h, 1).start()

    @pl.loop(0, CUTS)
    def _(h):
        pack(x_ref[:, span(h)], z, h)

    @pl.loop(0, 2 * CUTS * (planes - 1))
    def _(e):
        dist = lax.div(e, 2 * CUTS) + 1
        h = lax.rem(lax.div(e, 2), CUTS)
        side = lax.rem(e, 2)
        zs = z - dist + 2 * dist * side

        @pl.when((zs >= 0) & (zs < planes))
        def _():
            hop(zs, h, side).wait_recv()
            onward = z + 1 - 2 * side

            @pl.when((onward >= 0) & (onward < planes))
            def _():
                hop(zs, h, side).start()

            pack(toks[zs, :, span(h)], zs, h)

    @pl.loop(0, planes * CUTS)
    def _(e):
        zs = lax.div(e, CUTS)
        h = lax.rem(e, CUTS)

        @pl.when((zs <= z) & (z < planes - 1))
        def _():
            hop(zs, h, 0).wait_send()

        @pl.when((zs >= z) & (z > 0))
        def _():
            hop(zs, h, 1).wait_send()

        local_copy(zs, h).wait()
        for k in range(1, peers):
            other = lax.rem(p + k, peers)
            plane_copy(zs, h, other, p).wait_send()
            plane_copy(zs, h, other, other).wait_recv()


def return_kernel(
    planes, stride, tps, cap,
    y_ref, tab_ref, mid_ref, out_ref,
    held, part, from_low, from_high, zsend, lowrecv, highrecv, psend, precv, lsem, total,
):
    z, r, tp, p = place(stride, tps)
    peers = stride * tps
    rows, width = mid_ref.shape
    cols = width // CUTS
    slots = peers * cap
    greet(z, r, tp, p, planes, stride, tps)

    def span(h):
        return pl.ds(pl.multiple_of(h * cols, cols), cols)

    def plane_copy(zs, h, dest, at):
        return pltpu.make_async_remote_copy(
            src_ref=y_ref.at[zs, dest, :, span(h)],
            dst_ref=held.at[zs, pl.ds(pl.multiple_of(at * cap, cap), cap), span(h)],
            send_sem=psend.at[zs, h, dest],
            recv_sem=precv.at[zs, h, at],
            device_id=(z * stride + lax.div(dest, tps), lax.rem(dest, tps)),
            device_id_type=MESH,
        )

    def local_copy(zs, h):
        return pltpu.make_async_copy(
            y_ref.at[zs, p, :, span(h)],
            held.at[zs, pl.ds(pl.multiple_of(p * cap, cap), cap), span(h)],
            lsem.at[zs, h],
        )

    def send_out(zs, h):
        for k in range(1, peers):
            plane_copy(zs, h, lax.rem(p + k, peers), p).start()
        local_copy(zs, h).start()

    def up(zs, h):
        return pltpu.make_async_remote_copy(
            src_ref=part.at[zs, :, span(h)],
            dst_ref=from_low.at[zs, :, span(h)],
            send_sem=zsend.at[zs, h],
            recv_sem=lowrecv.at[zs, h],
            device_id=((z + 1) * stride + r, tp),
            device_id_type=MESH,
        )

    def down(zs, h):
        return pltpu.make_async_remote_copy(
            src_ref=part.at[zs, :, span(h)],
            dst_ref=from_high.at[zs, :, span(h)],
            send_sem=zsend.at[zs, h],
            recv_sem=highrecv.at[zs, h],
            device_id=((z - 1) * stride + r, tp),
            device_id_type=MESH,
        )

    def combined(zs, h):
        local_copy(zs, h).wait()
        for k in range(1, peers):
            plane_copy(zs, h, p, lax.rem(p + k, peers)).wait_recv()
        tab = tab_ref[lax.rem(z - zs + planes, planes)]
        first, second = slot_hits(tab, z, slots, rows)
        mix = jnp.where(first, tab[2:3, :], 0.0) + jnp.where(second, tab[3:4, :], 0.0)
        return jnp.dot(
            mix.T.astype(jnp.bfloat16), held[zs, :, span(h)], preferred_element_type=jnp.float32
        )

    events = 2 * CUTS * (planes - 1)

    def event(e):
        dist = planes - 1 - lax.div(e, 2 * CUTS)
        h = lax.rem(lax.div(e, 2), CUTS)
        side = lax.rem(e, 2)
        zs = z + dist - 2 * dist * side
        return zs, h, side

    @pl.loop(0, events)
    def _(e):
        zs, h, side = event(e)

        @pl.when((zs >= 0) & (zs < planes))
        def _():
            send_out(zs, h)

    @pl.loop(0, CUTS)
    def _(h):
        send_out(z, h)

    @pl.loop(0, events)
    def _(e):
        zs, h, side = event(e)

        @pl.when((zs >= 0) & (zs < planes))
        def _():
            mine = combined(zs, h)
            part[zs, :, span(h)] = mine.astype(jnp.bfloat16)

            @pl.when((side == 0) & (z > 0))
            def _():
                up(zs, h).wait_recv()
                part[zs, :, span(h)] = (
                    part[zs, :, span(h)].astype(jnp.float32)
                    + from_low[zs, :, span(h)].astype(jnp.float32)
                ).astype(jnp.bfloat16)

            @pl.when((side == 1) & (z < planes - 1))
            def _():
                down(zs, h).wait_recv()
                part[zs, :, span(h)] = (
                    part[zs, :, span(h)].astype(jnp.float32)
                    + from_high[zs, :, span(h)].astype(jnp.float32)
                ).astype(jnp.bfloat16)

            @pl.when(side == 0)
            def _():
                up(zs, h).start()

            @pl.when(side == 1)
            def _():
                down(zs, h).start()

    @pl.loop(0, CUTS)
    def _(h):
        total[:, span(h)] = mid_ref[:, span(h)].astype(jnp.float32) + combined(z, h)

        @pl.when(z > 0)
        def _():
            up(z, h).wait_recv()
            total[:, span(h)] += from_low[z, :, span(h)].astype(jnp.float32)

        @pl.when(z < planes - 1)
        def _():
            down(z, h).wait_recv()
            total[:, span(h)] += from_high[z, :, span(h)].astype(jnp.float32)

        out_ref[:, span(h)] = total[:, span(h)].astype(jnp.bfloat16)

    @pl.loop(0, planes * CUTS)
    def _(e):
        zs = lax.div(e, CUTS)
        h = lax.rem(e, CUTS)

        @pl.when(zs > z)
        def _():
            up(zs, h).wait_send()

        @pl.when(zs < z)
        def _():
            down(zs, h).wait_send()

        for k in range(1, peers):
            plane_copy(zs, h, lax.rem(p + k, peers), p).wait_send()


def routed_by_plane(normed, mid, tables, cap, weights):
    planes = tables.shape[0]
    rows, width = normed.shape
    tps = lax.axis_size("tp")
    stride = lax.axis_size("sp") // planes
    peers = stride * tps
    dma = pltpu.SemaphoreType.DMA
    vmem = pl.BlockSpec(memory_space=pltpu.VMEM)
    anywhere = pl.BlockSpec(memory_space=pl.ANY)
    arrived = pl.pallas_call(
        functools.partial(dispatch_kernel, planes, stride, tps, cap),
        out_shape=jax.ShapeDtypeStruct((planes, peers, cap, width), jnp.bfloat16),
        in_specs=[vmem, vmem],
        out_specs=anywhere,
        scratch_shapes=[
            pltpu.VMEM((planes, rows, width), jnp.bfloat16),
            pltpu.VMEM((planes, peers * cap, width), jnp.bfloat16),
            dma((2, planes, CUTS)),
            dma((planes, CUTS)),
            dma((planes, CUTS, peers)),
            dma((planes, CUTS, peers)),
            dma((planes, CUTS)),
        ],
        compiler_params=pltpu.CompilerParams(
            collective_id=0, has_side_effects=True, vmem_limit_bytes=32 * 1024 * 1024
        ),
        name="dispatch",
    )(normed, tables)
    finished = expert_rows(arrived, *weights)
    return pl.pallas_call(
        functools.partial(return_kernel, planes, stride, tps, cap),
        out_shape=jax.ShapeDtypeStruct((rows, width), jnp.bfloat16),
        in_specs=[anywhere, vmem, vmem],
        out_specs=vmem,
        scratch_shapes=[
            pltpu.VMEM((planes, peers * cap, width), jnp.bfloat16),
            pltpu.VMEM((planes, rows, width), jnp.bfloat16),
            pltpu.VMEM((planes, rows, width), jnp.bfloat16),
            pltpu.VMEM((planes, rows, width), jnp.bfloat16),
            dma((planes, CUTS)),
            dma((planes, CUTS)),
            dma((planes, CUTS)),
            dma((planes, CUTS, peers)),
            dma((planes, CUTS, peers)),
            dma((planes, CUTS)),
            pltpu.VMEM((rows, width), jnp.float32),
        ],
        compiler_params=pltpu.CompilerParams(
            collective_id=1, has_side_effects=True, vmem_limit_bytes=40 * 1024 * 1024
        ),
        name="combine",
    )(finished, tables, mid)


def expert_rows(arrived, gate_w, up_w, down_w):
    width = arrived.shape[-1]
    flat_rows = arrived.reshape(-1, width)
    gate = jnp.dot(flat_rows, gate_w, preferred_element_type=jnp.float32)
    upper = jnp.dot(flat_rows, up_w, preferred_element_type=jnp.float32)
    expert_hidden = (jax.nn.silu(gate) * upper).astype(jnp.bfloat16)
    result = jnp.dot(expert_hidden, down_w, preferred_element_type=jnp.float32).astype(jnp.bfloat16)
    return result.reshape(arrived.shape[:-1] + (result.shape[-1],))


def shards(
    queries,
    keys_values,
    doc_ids,
    head_sink,
    out_weight,
    hidden_in,
    norm_gain,
    expert_gate,
    expert_up,
    expert_down,
    routes,
    route_weight,
):
    tok_here = queries.shape[0]
    heads_here = head_sink.shape[0]
    kv_here = keys_values.shape[1]
    group = heads_here // kv_here
    head_dim = keys_values.shape[2] // 2
    docs_wide = jnp.broadcast_to(
        doc_ids.astype(jnp.bfloat16)[:, None], (tok_here, keys_values.shape[2])
    )
    slab = jnp.concatenate([keys_values.reshape(tok_here, -1), docs_wide], axis=1)
    slab = with_halo(slab, "sp", WIN)
    kv_ext = slab[:, : kv_here * keys_values.shape[2]].reshape(
        -1, kv_here, keys_values.shape[2]
    )
    docs_ext = slab[:, kv_here * keys_values.shape[2]].astype(jnp.int32)
    offset = lax.axis_index("sp") * tok_here
    seq_total = lax.axis_size("sp") * tok_here
    span_rows = min(512, tok_here)
    sink_logit = head_sink.reshape(kv_here, group)[:, :, None, None]

    def one_span(span_index):
        first_row = span_index * span_rows
        q_span = queries.reshape(span_rows, kv_here, group, head_dim)
        scores = jnp.einsum(
            "qhgd,khd->hgqk", q_span, kv_ext[..., :head_dim], preferred_element_type=jnp.float32
        ) * HD ** (-0.5)
        query_pos = offset + first_row + jnp.arange(span_rows, dtype=jnp.int32)
        key_pos = offset + first_row - WIN + jnp.arange(span_rows + 2 * WIN, dtype=jnp.int32)
        inside = (key_pos >= 0) & (key_pos < seq_total)
        allowed = (
            (jnp.abs(key_pos[None, :] - query_pos[:, None]) <= WIN)
            & inside[None, :]
            & (docs_ext[None, :] == doc_ids[:, None])
        )
        masked = jnp.where(allowed, scores, -1e30)
        row_max = jnp.maximum(masked.max(-1, keepdims=True), sink_logit)
        exp_scores = jnp.where(allowed, jnp.exp(masked - row_max), 0.0)
        total_mass = exp_scores.sum(-1, keepdims=True) + jnp.exp(sink_logit - row_max)
        weights = (exp_scores / total_mass).astype(jnp.bfloat16)
        outcome = jnp.einsum(
            "hgqk,khd->qhgd", weights, kv_ext[..., head_dim:], preferred_element_type=jnp.float32
        )
        return outcome.astype(jnp.bfloat16).reshape(span_rows, heads_here * head_dim)

    attended = lax.map(one_span, jnp.arange(tok_here // span_rows, dtype=jnp.int32)).reshape(
        tok_here, -1
    )
    if lax.axis_size("tp") == 2:
        tp = lax.axis_index("tp")
        half = tok_here // 2
        mine = lax.dynamic_slice_in_dim(attended, tp * half, half, 0)
        other = lax.ppermute(
            lax.dynamic_slice_in_dim(attended, (1 - tp) * half, half, 0), "tp", [(0, 1), (1, 0)]
        )
        gathered = jnp.concatenate(
            [jnp.where(tp == 0, mine, other), jnp.where(tp == 0, other, mine)], axis=1
        )
    else:
        gathered = lax.all_to_all(attended, "tp", split_axis=0, concat_axis=1, tiled=True)
    projected = jnp.dot(gathered, out_weight, preferred_element_type=jnp.float32)
    mid_wide = (hidden_in.astype(jnp.float32) + projected).astype(jnp.bfloat16).astype(jnp.float32)
    normed = (
        mid_wide
        * lax.rsqrt(jnp.mean(mid_wide * mid_wide, axis=-1, keepdims=True) + 1e-06)
        * norm_gain
    ).astype(jnp.bfloat16)
    local_rows = normed.shape[0]
    topk = routes.shape[1]
    width = normed.shape[1]
    sp_count = lax.axis_size("sp")
    tp_count = lax.axis_size("tp")
    expert_count = sp_count * tp_count
    capacity = 2 * local_rows * topk // expert_count
    flat_routes = routes.reshape(-1)
    one_hot = (flat_routes[:, None] == jnp.arange(expert_count, dtype=jnp.int32)[None, :]).astype(
        jnp.int32
    )
    slot_rank = (jnp.cumsum(one_hot, axis=0) * one_hot).sum(-1) - 1
    slot_index = flat_routes * capacity + slot_rank
    if capacity % 16 == 0 and sp_count % PLANES == 0 and topk == 2:
        tab = jnp.concatenate(
            [
                slot_index.reshape(local_rows, topk).astype(jnp.float32).T,
                route_weight.T,
                jnp.zeros((4, local_rows), jnp.float32),
            ],
            axis=0,
        )
        stride = sp_count // PLANES
        tables = jnp.stack(
            [tab]
            + [
                lax.ppermute(
                    tab, "sp", [(i, (i + d * stride) % sp_count) for i in range(sp_count)]
                )
                for d in range(1, PLANES)
            ]
        )
        return routed_by_plane(
            normed,
            mid_wide.astype(jnp.bfloat16),
            tables,
            capacity,
            (expert_gate[0], expert_up[0], expert_down[0]),
        )
    repeated = jnp.repeat(normed, topk, axis=0)
    buffer_rows = (
        jnp.zeros((expert_count * capacity, width), jnp.bfloat16).at[slot_index].set(repeated)
    )
    sent = buffer_rows.reshape(expert_count, capacity, width)
    finished = expert_rows(
        lax.all_to_all(sent, ("sp", "tp"), split_axis=0, concat_axis=0, tiled=True),
        expert_gate[0],
        expert_up[0],
        expert_down[0],
    )
    returned = lax.all_to_all(finished, ("sp", "tp"), split_axis=0, concat_axis=0, tiled=True)
    returned = returned.reshape(expert_count * capacity, width)
    picked = returned[slot_index].astype(jnp.float32).reshape(local_rows, topk, width)
    mixture = jnp.sum(picked * route_weight[..., None], axis=1)
    return (mid_wide + mixture).astype(jnp.bfloat16)


def solution(mesh):
    placed = (
        P("sp", "tp"),
        P("sp", "tp", None),
        P("sp"),
        P("tp"),
        P(),
        P(("sp", "tp"), None),
        P(),
        P(("sp", "tp"), None, None),
        P(("sp", "tp"), None, None),
        P(("sp", "tp"), None, None),
        P(("sp", "tp"), None),
        P(("sp", "tp"), None),
    )
    return jax.shard_map(
        shards, mesh=mesh, in_specs=placed, out_specs=P(("sp", "tp"), None), check_vma=False
    )
```

```python
import functools

import jax
import jax.numpy as jnp
from jax import lax
from jax.experimental import pallas as pl
from jax.experimental.pallas import tpu as pltpu
from jax.sharding import PartitionSpec as P

HD = 64
WIN = 128
PLANES = 4
CUTS = 4
TILE = 256
MESH = pl.DeviceIdType.MESH


def with_halo(cells, axis, width):
    count = lax.axis_size(axis)
    ends = count - 1
    return jnp.concatenate(
        [
            lax.ppermute(cells[-width:], axis, [(i, (i + 1) % count) for i in range(ends)]),
            cells,
            lax.ppermute(cells[:width], axis, [((i + 1) % count, i) for i in range(ends)]),
        ],
        axis=0,
    )


def place(stride, tps):
    sp = lax.axis_index("sp")
    tp = lax.axis_index("tp")
    return lax.div(sp, stride), lax.rem(sp, stride), tp, lax.rem(sp, stride) * tps + tp


def greet(z, r, tp, p, planes, stride, tps):
    peers = stride * tps
    barrier = pltpu.get_barrier_semaphore()
    for k in range(1, peers):
        pd = lax.rem(p + k, peers)
        pl.semaphore_signal(
            barrier,
            inc=1,
            device_id=(z * stride + lax.div(pd, tps), lax.rem(pd, tps)),
            device_id_type=MESH,
        )

    @pl.when(z > 0)
    def _():
        pl.semaphore_signal(
            barrier, inc=1, device_id=((z - 1) * stride + r, tp), device_id_type=MESH
        )

    @pl.when(z < planes - 1)
    def _():
        pl.semaphore_signal(
            barrier, inc=1, device_id=((z + 1) * stride + r, tp), device_id_type=MESH
        )

    beside = (z > 0).astype(jnp.int32) + (z < planes - 1).astype(jnp.int32)
    pl.semaphore_wait(barrier, peers - 1 + beside)


def slot_hits(tab, z, slots, rows):
    ids = lax.broadcasted_iota(jnp.int32, (slots, rows), 0) + z * slots
    ids = ids.astype(jnp.float32)
    return ids == tab[0:1, :], ids == tab[1:2, :]


def dispatch_kernel(
    planes, stride, tps, cap,
    x_ref, tab_ref, gate_ref, up_ref, down_ref, out_ref, tab_out,
    toks, stage, zsend, zrecv, psend, precv, lsem,
    land, results, hidden, gate_w, up_w, down_w, tabs, tsend, trecv, wsem, ysem,
):
    z, r, tp, p = place(stride, tps)
    peers = stride * tps
    rows, width = x_ref.shape
    cols = width // CUTS
    slots = peers * cap
    greet(z, r, tp, p, planes, stride, tps)

    def span(h):
        return pl.ds(pl.multiple_of(h * cols, cols), cols)

    def hop(zs, h, side):
        return pltpu.make_async_remote_copy(
            src_ref=toks.at[zs, :, span(h)],
            dst_ref=toks.at[zs, :, span(h)],
            send_sem=zsend.at[side, zs, h],
            recv_sem=zrecv.at[zs, h],
            device_id=((z + 1 - 2 * side) * stride + r, tp),
            device_id_type=MESH,
        )

    def own_hop(h, side):
        return pltpu.make_async_remote_copy(
            src_ref=x_ref.at[:, span(h)],
            dst_ref=toks.at[z, :, span(h)],
            send_sem=zsend.at[side, z, h],
            recv_sem=zrecv.at[z, h],
            device_id=((z + 1 - 2 * side) * stride + r, tp),
            device_id_type=MESH,
        )

    def plane_copy(zs, h, dest, at):
        return pltpu.make_async_remote_copy(
            src_ref=stage.at[zs, pl.ds(pl.multiple_of(dest * cap, cap), cap), span(h)],
            dst_ref=land.at[zs, pl.ds(pl.multiple_of(at * cap, cap), cap), span(h)],
            send_sem=psend.at[zs, h, dest],
            recv_sem=precv.at[zs, h, at],
            device_id=(z * stride + lax.div(dest, tps), lax.rem(dest, tps)),
            device_id_type=MESH,
        )

    def local_copy(zs, h):
        return pltpu.make_async_copy(
            stage.at[zs, pl.ds(pl.multiple_of(p * cap, cap), cap), span(h)],
            land.at[zs, pl.ds(pl.multiple_of(p * cap, cap), cap), span(h)],
            lsem.at[zs, h],
        )

    def tab_hop(zs, side, source):
        return pltpu.make_async_remote_copy(
            src_ref=source,
            dst_ref=tabs.at[zs],
            send_sem=tsend.at[side, zs],
            recv_sem=trecv.at[zs],
            device_id=((z + 1 - 2 * side) * stride + r, tp),
            device_id_type=MESH,
        )

    loads = [
        pltpu.make_async_copy(source, target, wsem.at[k])
        for k, (source, target) in enumerate(
            [(gate_ref, gate_w), (up_ref, up_w), (down_ref, down_w)]
        )
    ]

    def result_copy(zs):
        return pltpu.make_async_copy(results.at[zs], out_ref.at[zs], ysem.at[zs])

    def experts(zs):
        @pl.loop(0, CUTS)
        def _(h):
            local_copy(zs, h).wait()
            for k in range(1, peers):
                other = lax.rem(p + k, peers)
                plane_copy(zs, h, other, other).wait_recv()

        @pl.loop(0, gate_w.shape[1] // TILE)
        def _(c):
            at = pl.ds(pl.multiple_of(c * TILE, TILE), TILE)
            gate = jnp.dot(land[zs], gate_w[:, at], preferred_element_type=jnp.float32)
            upper = jnp.dot(land[zs], up_w[:, at], preferred_element_type=jnp.float32)
            hidden[:, at] = (gate / (1.0 + jnp.exp(-gate)) * upper).astype(jnp.bfloat16)

        @pl.loop(0, width // TILE)
        def _(c):
            at = pl.ds(pl.multiple_of(c * TILE, TILE), TILE)
            results[zs, :, at] = jnp.dot(
                hidden[...], down_w[:, at], preferred_element_type=jnp.float32
            ).astype(jnp.bfloat16)

        result_copy(zs).start()

    def experts_at(dist):
        @pl.loop(0, 2)
        def _(side):
            zs = z - dist + 2 * dist * side

            @pl.when((zs >= 0) & (zs < planes) & ((dist > 0) | (side == 0)))
            def _():
                experts(zs)

    def pack(block, zs, h):
        first, second = slot_hits(tabs[zs], z, slots, rows)
        pick = jnp.where(first | second, 1.0, 0.0).astype(jnp.bfloat16)
        stage[zs, :, span(h)] = jnp.dot(
            pick, block, preferred_element_type=jnp.float32
        ).astype(jnp.bfloat16)
        for k in range(1, peers):
            plane_copy(zs, h, lax.rem(p + k, peers), p).start()
        local_copy(zs, h).start()

    @pl.when(z < planes - 1)
    def _():
        tab_hop(z, 0, tab_ref).start()

    @pl.when(z > 0)
    def _():
        tab_hop(z, 1, tab_ref).start()

    for h in range(CUTS):

        @pl.when(z < planes - 1)
        def _():
            own_hop(h, 0).start()

        @pl.when(z > 0)
        def _():
            own_hop(h, 1).start()

    for load in loads:
        load.start()
    tabs[z] = tab_ref[...]

    @pl.loop(0, CUTS)
    def _(h):
        pack(x_ref[:, span(h)], z, h)

    for load in loads:
        load.wait()

    @pl.loop(0, 2 * CUTS * (planes - 1))
    def _(e):
        dist = lax.div(e, 2 * CUTS) + 1
        h = lax.rem(lax.div(e, 2), CUTS)
        side = lax.rem(e, 2)
        zs = z - dist + 2 * dist * side

        @pl.when((zs >= 0) & (zs < planes))
        def _():
            onward = z + 1 - 2 * side

            @pl.when(h == 0)
            def _():
                tab_hop(zs, side, tabs.at[zs]).wait_recv()

                @pl.when((onward >= 0) & (onward < planes))
                def _():
                    tab_hop(zs, side, tabs.at[zs]).start()

            hop(zs, h, side).wait_recv()

            @pl.when((onward >= 0) & (onward < planes))
            def _():
                hop(zs, h, side).start()

            pack(toks[zs, :, span(h)], zs, h)

        @pl.when((side == 1) & (h == CUTS // 2 - 1))
        def _():
            experts_at(dist - 1)

    experts_at(planes - 1)

    @pl.loop(0, planes * CUTS)
    def _(e):
        zs = lax.div(e, CUTS)
        h = lax.rem(e, CUTS)

        @pl.when((zs <= z) & (z < planes - 1))
        def _():
            hop(zs, h, 0).wait_send()

        @pl.when((zs >= z) & (z > 0))
        def _():
            hop(zs, h, 1).wait_send()

        for k in range(1, peers):
            plane_copy(zs, h, lax.rem(p + k, peers), p).wait_send()

    @pl.loop(0, planes)
    def _(zs):
        @pl.when((zs <= z) & (z < planes - 1))
        def _():
            tab_hop(zs, 0, tabs.at[zs]).wait_send()

        @pl.when((zs >= z) & (z > 0))
        def _():
            tab_hop(zs, 1, tabs.at[zs]).wait_send()

        result_copy(zs).wait()

    tab_out[...] = tabs[...]


def return_kernel(
    planes, stride, tps, cap,
    y_ref, tab_ref, mid_ref, out_ref,
    held, part, from_low, from_high, zsend, lowrecv, highrecv, psend, precv, lsem, total,
):
    z, r, tp, p = place(stride, tps)
    peers = stride * tps
    rows, width = mid_ref.shape
    cols = width // CUTS
    slots = peers * cap
    greet(z, r, tp, p, planes, stride, tps)

    def span(h):
        return pl.ds(pl.multiple_of(h * cols, cols), cols)

    def plane_copy(zs, h, dest, at):
        return pltpu.make_async_remote_copy(
            src_ref=y_ref.at[zs, pl.ds(pl.multiple_of(dest * cap, cap), cap), span(h)],
            dst_ref=held.at[zs, pl.ds(pl.multiple_of(at * cap, cap), cap), span(h)],
            send_sem=psend.at[zs, h, dest],
            recv_sem=precv.at[zs, h, at],
            device_id=(z * stride + lax.div(dest, tps), lax.rem(dest, tps)),
            device_id_type=MESH,
        )

    def local_copy(zs, h):
        return pltpu.make_async_copy(
            y_ref.at[zs, pl.ds(pl.multiple_of(p * cap, cap), cap), span(h)],
            held.at[zs, pl.ds(pl.multiple_of(p * cap, cap), cap), span(h)],
            lsem.at[zs, h],
        )

    def send_out(zs, h):
        for k in range(1, peers):
            plane_copy(zs, h, lax.rem(p + k, peers), p).start()
        local_copy(zs, h).start()

    def up(zs, h):
        return pltpu.make_async_remote_copy(
            src_ref=part.at[zs, :, span(h)],
            dst_ref=from_low.at[zs, :, span(h)],
            send_sem=zsend.at[zs, h],
            recv_sem=lowrecv.at[zs, h],
            device_id=((z + 1) * stride + r, tp),
            device_id_type=MESH,
        )

    def down(zs, h):
        return pltpu.make_async_remote_copy(
            src_ref=part.at[zs, :, span(h)],
            dst_ref=from_high.at[zs, :, span(h)],
            send_sem=zsend.at[zs, h],
            recv_sem=highrecv.at[zs, h],
            device_id=((z - 1) * stride + r, tp),
            device_id_type=MESH,
        )

    def combined(zs, h):
        local_copy(zs, h).wait()
        for k in range(1, peers):
            plane_copy(zs, h, p, lax.rem(p + k, peers)).wait_recv()
        tab = tab_ref[zs]
        first, second = slot_hits(tab, z, slots, rows)
        mix = jnp.where(first, tab[2:3, :], 0.0) + jnp.where(second, tab[3:4, :], 0.0)
        return jnp.dot(
            mix.T.astype(jnp.bfloat16), held[zs, :, span(h)], preferred_element_type=jnp.float32
        )

    events = 2 * CUTS * (planes - 1)

    def event(e):
        dist = planes - 1 - lax.div(e, 2 * CUTS)
        h = lax.rem(lax.div(e, 2), CUTS)
        side = lax.rem(e, 2)
        zs = z + dist - 2 * dist * side
        return zs, h, side

    @pl.loop(0, events)
    def _(e):
        zs, h, side = event(e)

        @pl.when((zs >= 0) & (zs < planes))
        def _():
            send_out(zs, h)

    @pl.loop(0, CUTS)
    def _(h):
        send_out(z, h)

    @pl.loop(0, events)
    def _(e):
        zs, h, side = event(e)

        @pl.when((zs >= 0) & (zs < planes))
        def _():
            mine = combined(zs, h)
            part[zs, :, span(h)] = mine.astype(jnp.bfloat16)

            @pl.when((side == 0) & (z > 0))
            def _():
                up(zs, h).wait_recv()
                part[zs, :, span(h)] = (
                    part[zs, :, span(h)].astype(jnp.float32)
                    + from_low[zs, :, span(h)].astype(jnp.float32)
                ).astype(jnp.bfloat16)

            @pl.when((side == 1) & (z < planes - 1))
            def _():
                down(zs, h).wait_recv()
                part[zs, :, span(h)] = (
                    part[zs, :, span(h)].astype(jnp.float32)
                    + from_high[zs, :, span(h)].astype(jnp.float32)
                ).astype(jnp.bfloat16)

            @pl.when(side == 0)
            def _():
                up(zs, h).start()

            @pl.when(side == 1)
            def _():
                down(zs, h).start()

    @pl.loop(0, CUTS)
    def _(h):
        total[:, span(h)] = mid_ref[:, span(h)].astype(jnp.float32) + combined(z, h)

        @pl.when(z > 0)
        def _():
            up(z, h).wait_recv()
            total[:, span(h)] += from_low[z, :, span(h)].astype(jnp.float32)

        @pl.when(z < planes - 1)
        def _():
            down(z, h).wait_recv()
            total[:, span(h)] += from_high[z, :, span(h)].astype(jnp.float32)

        out_ref[:, span(h)] = total[:, span(h)].astype(jnp.bfloat16)

    @pl.loop(0, planes * CUTS)
    def _(e):
        zs = lax.div(e, CUTS)
        h = lax.rem(e, CUTS)

        @pl.when(zs > z)
        def _():
            up(zs, h).wait_send()

        @pl.when(zs < z)
        def _():
            down(zs, h).wait_send()

        for k in range(1, peers):
            plane_copy(zs, h, lax.rem(p + k, peers), p).wait_send()


def routed_by_plane(normed, mid, tab, planes, cap, weights):
    rows, width = normed.shape
    tps = lax.axis_size("tp")
    stride = lax.axis_size("sp") // planes
    peers = stride * tps
    dma = pltpu.SemaphoreType.DMA
    vmem = pl.BlockSpec(memory_space=pltpu.VMEM)
    anywhere = pl.BlockSpec(memory_space=pl.ANY)
    hidden = weights[0].shape[1]
    finished, tables = pl.pallas_call(
        functools.partial(dispatch_kernel, planes, stride, tps, cap),
        out_shape=[
            jax.ShapeDtypeStruct((planes, peers * cap, width), jnp.bfloat16),
            jax.ShapeDtypeStruct((planes,) + tab.shape, jnp.float32),
        ],
        in_specs=[vmem, vmem, anywhere, anywhere, anywhere],
        out_specs=[anywhere, vmem],
        scratch_shapes=[
            pltpu.VMEM((planes, rows, width), jnp.bfloat16),
            pltpu.VMEM((planes, peers * cap, width), jnp.bfloat16),
            dma((2, planes, CUTS)),
            dma((planes, CUTS)),
            dma((planes, CUTS, peers)),
            dma((planes, CUTS, peers)),
            dma((planes, CUTS)),
            pltpu.VMEM((planes, peers * cap, width), jnp.bfloat16),
            pltpu.VMEM((planes, peers * cap, width), jnp.bfloat16),
            pltpu.VMEM((peers * cap, hidden), jnp.bfloat16),
            pltpu.VMEM((width, hidden), jnp.bfloat16),
            pltpu.VMEM((width, hidden), jnp.bfloat16),
            pltpu.VMEM((hidden, width), jnp.bfloat16),
            pltpu.VMEM((planes,) + tab.shape, jnp.float32),
            dma((2, planes)),
            dma((planes,)),
            dma((3,)),
            dma((planes,)),
        ],
        compiler_params=pltpu.CompilerParams(
            collective_id=0, has_side_effects=True, vmem_limit_bytes=48 * 1024 * 1024
        ),
        name="dispatch",
    )(normed, tab, *weights)
    return pl.pallas_call(
        functools.partial(return_kernel, planes, stride, tps, cap),
        out_shape=jax.ShapeDtypeStruct((rows, width), jnp.bfloat16),
        in_specs=[anywhere, vmem, vmem],
        out_specs=vmem,
        scratch_shapes=[
            pltpu.VMEM((planes, peers * cap, width), jnp.bfloat16),
            pltpu.VMEM((planes, rows, width), jnp.bfloat16),
            pltpu.VMEM((planes, rows, width), jnp.bfloat16),
            pltpu.VMEM((planes, rows, width), jnp.bfloat16),
            dma((planes, CUTS)),
            dma((planes, CUTS)),
            dma((planes, CUTS)),
            dma((planes, CUTS, peers)),
            dma((planes, CUTS, peers)),
            dma((planes, CUTS)),
            pltpu.VMEM((rows, width), jnp.float32),
        ],
        compiler_params=pltpu.CompilerParams(
            collective_id=1, has_side_effects=True, vmem_limit_bytes=40 * 1024 * 1024
        ),
        name="combine",
    )(finished, tables, mid)


def expert_rows(arrived, gate_w, up_w, down_w):
    width = arrived.shape[-1]
    flat_rows = arrived.reshape(-1, width)
    gate = jnp.dot(flat_rows, gate_w, preferred_element_type=jnp.float32)
    upper = jnp.dot(flat_rows, up_w, preferred_element_type=jnp.float32)
    expert_hidden = (jax.nn.silu(gate) * upper).astype(jnp.bfloat16)
    result = jnp.dot(expert_hidden, down_w, preferred_element_type=jnp.float32).astype(jnp.bfloat16)
    return result.reshape(arrived.shape[:-1] + (result.shape[-1],))


def shards(
    queries,
    keys_values,
    doc_ids,
    head_sink,
    out_weight,
    hidden_in,
    norm_gain,
    expert_gate,
    expert_up,
    expert_down,
    routes,
    route_weight,
):
    tok_here = queries.shape[0]
    heads_here = head_sink.shape[0]
    kv_here = keys_values.shape[1]
    group = heads_here // kv_here
    head_dim = keys_values.shape[2] // 2
    docs_wide = jnp.broadcast_to(
        doc_ids.astype(jnp.bfloat16)[:, None], (tok_here, keys_values.shape[2])
    )
    slab = jnp.concatenate([keys_values.reshape(tok_here, -1), docs_wide], axis=1)
    slab = with_halo(slab, "sp", WIN)
    kv_ext = slab[:, : kv_here * keys_values.shape[2]].reshape(
        -1, kv_here, keys_values.shape[2]
    )
    docs_ext = slab[:, kv_here * keys_values.shape[2]].astype(jnp.int32)
    offset = lax.axis_index("sp") * tok_here
    seq_total = lax.axis_size("sp") * tok_here
    span_rows = min(512, tok_here)
    sink_logit = head_sink.reshape(kv_here, group)[:, :, None, None]

    def one_span(span_index):
        first_row = span_index * span_rows
        q_span = queries.reshape(span_rows, kv_here, group, head_dim)
        scores = jnp.einsum(
            "qhgd,khd->hgqk", q_span, kv_ext[..., :head_dim], preferred_element_type=jnp.float32
        ) * HD ** (-0.5)
        query_pos = offset + first_row + jnp.arange(span_rows, dtype=jnp.int32)
        key_pos = offset + first_row - WIN + jnp.arange(span_rows + 2 * WIN, dtype=jnp.int32)
        inside = (key_pos >= 0) & (key_pos < seq_total)
        allowed = (
            (jnp.abs(key_pos[None, :] - query_pos[:, None]) <= WIN)
            & inside[None, :]
            & (docs_ext[None, :] == doc_ids[:, None])
        )
        masked = jnp.where(allowed, scores, -1e30)
        row_max = jnp.maximum(masked.max(-1, keepdims=True), sink_logit)
        exp_scores = jnp.where(allowed, jnp.exp(masked - row_max), 0.0)
        total_mass = exp_scores.sum(-1, keepdims=True) + jnp.exp(sink_logit - row_max)
        weights = (exp_scores / total_mass).astype(jnp.bfloat16)
        outcome = jnp.einsum(
            "hgqk,khd->qhgd", weights, kv_ext[..., head_dim:], preferred_element_type=jnp.float32
        )
        return outcome.astype(jnp.bfloat16).reshape(span_rows, heads_here * head_dim)

    attended = lax.map(one_span, jnp.arange(tok_here // span_rows, dtype=jnp.int32)).reshape(
        tok_here, -1
    )
    if lax.axis_size("tp") == 2:
        tp = lax.axis_index("tp")
        half = tok_here // 2
        mine = lax.dynamic_slice_in_dim(attended, tp * half, half, 0)
        other = lax.ppermute(
            lax.dynamic_slice_in_dim(attended, (1 - tp) * half, half, 0), "tp", [(0, 1), (1, 0)]
        )
        gathered = jnp.concatenate(
            [jnp.where(tp == 0, mine, other), jnp.where(tp == 0, other, mine)], axis=1
        )
    else:
        gathered = lax.all_to_all(attended, "tp", split_axis=0, concat_axis=1, tiled=True)
    projected = jnp.dot(gathered, out_weight, preferred_element_type=jnp.float32)
    mid_wide = (hidden_in.astype(jnp.float32) + projected).astype(jnp.bfloat16).astype(jnp.float32)
    normed = (
        mid_wide
        * lax.rsqrt(jnp.mean(mid_wide * mid_wide, axis=-1, keepdims=True) + 1e-06)
        * norm_gain
    ).astype(jnp.bfloat16)
    local_rows = normed.shape[0]
    topk = routes.shape[1]
    width = normed.shape[1]
    sp_count = lax.axis_size("sp")
    tp_count = lax.axis_size("tp")
    expert_count = sp_count * tp_count
    capacity = 2 * local_rows * topk // expert_count
    flat_routes = routes.reshape(-1)
    one_hot = (flat_routes[:, None] == jnp.arange(expert_count, dtype=jnp.int32)[None, :]).astype(
        jnp.int32
    )
    slot_rank = (jnp.cumsum(one_hot, axis=0) * one_hot).sum(-1) - 1
    slot_index = flat_routes * capacity + slot_rank
    if capacity % 16 == 0 and sp_count % PLANES == 0 and topk == 2:
        tab = jnp.concatenate(
            [
                slot_index.reshape(local_rows, topk).astype(jnp.float32).T,
                route_weight.T,
                jnp.zeros((4, local_rows), jnp.float32),
            ],
            axis=0,
        )
        return routed_by_plane(
            normed,
            mid_wide.astype(jnp.bfloat16),
            tab,
            PLANES,
            capacity,
            (expert_gate[0], expert_up[0], expert_down[0]),
        )
    repeated = jnp.repeat(normed, topk, axis=0)
    buffer_rows = (
        jnp.zeros((expert_count * capacity, width), jnp.bfloat16).at[slot_index].set(repeated)
    )
    sent = buffer_rows.reshape(expert_count, capacity, width)
    finished = expert_rows(
        lax.all_to_all(sent, ("sp", "tp"), split_axis=0, concat_axis=0, tiled=True),
        expert_gate[0],
        expert_up[0],
        expert_down[0],
    )
    returned = lax.all_to_all(finished, ("sp", "tp"), split_axis=0, concat_axis=0, tiled=True)
    returned = returned.reshape(expert_count * capacity, width)
    picked = returned[slot_index].astype(jnp.float32).reshape(local_rows, topk, width)
    mixture = jnp.sum(picked * route_weight[..., None], axis=1)
    return (mid_wide + mixture).astype(jnp.bfloat16)


def solution(mesh):
    placed = (
        P("sp", "tp"),
        P("sp", "tp", None),
        P("sp"),
        P("tp"),
        P(),
        P(("sp", "tp"), None),
        P(),
        P(("sp", "tp"), None, None),
        P(("sp", "tp"), None, None),
        P(("sp", "tp"), None, None),
        P(("sp", "tp"), None),
        P(("sp", "tp"), None),
    )
    return jax.shard_map(
        shards, mesh=mesh, in_specs=placed, out_specs=P(("sp", "tp"), None), check_vma=False
    )
```
